32 devices in a mesh: sp: 8 (over z, y), tp: 4 (over x, core).
Axes of the slice: x: 2, y: 2, z: 4, core: 2. Of those that a mesh axis runs over, the one named last changes fastest.
Arguments:
- inputs: bfloat16 [2, 1024, 2048], P(None, 'sp'), may hold values from -6 to 6
- norm_gain: float32 [2048], replicated, may hold values from 0.1 to 1.9
- query_weight: bfloat16 [2048, 1024], P('sp', 'tp'), may hold values from -0.125 to 0.125
- key_weight: bfloat16 [2048, 256], P('sp', 'tp'), may hold values from -0.125 to 0.125
- value_weight: bfloat16 [2048, 256], P('sp', 'tp'), may hold values from -0.125 to 0.125
- query_gain: float32 [64], replicated, may hold values from 0.1 to 24
- key_gain: float32 [64], replicated, may hold values from 0.1 to 1.9
- forget_cache: float32 [2, 16, 1024], P(None, 'tp'), may hold values from -104 to 0, as said below
- rec_in_weight: bfloat16 [2048, 1024], P('sp', 'tp'), may hold values from -0.125 to 0.125
- rec_gate_weight: bfloat16 [2048, 1024], P('sp', 'tp'), may hold values from -0.125 to 0.125
- conv_weight: bfloat16 [4, 1024], P(None, 'tp'), may hold values from -3 to 3
- decay_gate_weight: bfloat16 [16, 64, 64], P('tp'), may hold values from -0.75 to 0.75
- input_gate_weight: bfloat16 [16, 64, 64], P('tp'), may hold values from -0.75 to 0.75
- decay_param: float32 [1024], P('tp'), may hold values from 4 to 16
- decay_extra: float32 [2, 1024, 1024], P(None, 'sp', 'tp'), may hold values from -2 to 0
- attn_out_gain: float32 [1024], P('tp'), may hold values from 0.1 to 1.9
- rec_out_gain: float32 [1024], P('tp'), may hold values from 0.1 to 1.9
- out_att_weight: bfloat16 [1024, 2048], P('tp'), may hold values from -0.125 to 0.125
- out_rec_weight: bfloat16 [1024, 2048], P('tp'), may hold values from -0.125 to 0.125
Outputs:
- mixed: bfloat16 [2, 1024, 2048], P(None, 'sp', 'tp')
The draws below stay inside these ranges and needn't reach their ends.
Inputs may be any that keep to these rules, and one draw needn't show every extreme that they name: `forget_cache`: Non-increasing along the positions of each sequence and head.
All inputs are finite; a program needn't handle non-finite values.
Results may differ from the reference program's by a relative error of at most 0.012.
The reference program's roundings to bfloat16 on the way count: a program that leaves them out, or rounds other values in their place, can miss the bound.
Values may be sent and summed in bfloat16 or wider, within the bound.
A program may use at most 128 MiB of HBM per device.

```python
import math
import jax
import jax.numpy as jnp
from jax import lax

D = 2048
HEAD_DIM = 64
ATT_HEADS = 16
KV_HEADS = 4
LRU_BLOCK = 64
CONV_TAPS = 4
SEQS = 2
SEQ_TOK = 128
SEQUENCE_LENGTH = 1024
ATT_WIDTH = 1024
KV_WIDTH = 256
LRU_WIDTH = 1024
LRU_BLOCKS = 16


lru_const = 8.0


def spike_log_values(key, total_count):
    key_rows = jax.random.split(key, 2)
    spots = jax.random.randint(key_rows[0], (SEQS, total_count), 0, SEQUENCE_LENGTH)
    kept = jax.random.uniform(key_rows[1], (SEQS, total_count), jnp.float32, 0.5, 0.8)
    hits = (jnp.arange(SEQUENCE_LENGTH)[None, None, :] == spots[:, :, None]).astype(jnp.float32)
    return jnp.sum(hits * jnp.log(kept)[:, :, None], axis=1)


def block_factor(key):
    blocks = SEQUENCE_LENGTH // SEQ_TOK
    multiplier = jnp.exp(jax.random.uniform(key, (SEQS, blocks), jnp.float32, math.log(0.5), math.log(2.0)))
    return jnp.repeat(multiplier, SEQ_TOK, axis=1)


def draw_query_gain(key, part):
    key = jax.random.fold_in(key, 3)
    return 1.0 + 0.18 * jnp.clip(jax.random.normal(key, (HEAD_DIM,), jnp.float32), -4.5, 4.5)


def draw_forget_cache(key, part):
    key_rows = jax.random.split(jax.random.fold_in(key, 7), 6)
    order = jax.random.permutation(key_rows[0], ATT_HEADS)
    slow_rate = 0.6 / SEQUENCE_LENGTH * jax.random.uniform(key_rows[1], (ATT_HEADS,), jnp.float32, 0.5, 1.5)
    fast_len = jnp.exp(jax.random.uniform(key_rows[2], (ATT_HEADS,), jnp.float32, math.log(30.0), math.log(100.0)))
    decay_speed = jnp.where(order < ATT_HEADS // 2, 1.0 / fast_len, slow_rate)
    random_jitter = jax.random.uniform(key_rows[4], (SEQS, ATT_HEADS, SEQUENCE_LENGTH), jnp.float32, 0.5, 1.5)
    multiplier = block_factor(key_rows[3])
    gate_logarithm = -decay_speed[None, :, None] * multiplier[:, None, :] * random_jitter + spike_log_values(key_rows[5], 2)[:, None, :]
    return jnp.cumsum(gate_logarithm, axis=2)


def draw_decay_param(key, part):
    key_rows = jax.random.split(jax.random.fold_in(key, 5), 3)
    order = jax.random.permutation(key_rows[0], LRU_WIDTH)
    slow_rate = 0.3 / (lru_const * SEQUENCE_LENGTH) * jax.random.uniform(key_rows[1], (LRU_WIDTH,), jnp.float32, 0.5, 1.5)
    fast_len = jnp.exp(jax.random.uniform(key_rows[2], (LRU_WIDTH,), jnp.float32, math.log(30.0), math.log(100.0)))
    fast_rate = 1.0 / (0.5 * lru_const * fast_len)
    decay_speed = jnp.where(order < LRU_WIDTH // 2, fast_rate, slow_rate)
    return -jnp.log(jnp.expm1(decay_speed))


def draw_decay_extra(key, part):
    key_rows = jax.random.split(jax.random.fold_in(key, 9), 3)
    multiplier = block_factor(key_rows[0])
    random_jitter = jax.random.uniform(key_rows[1], (SEQS, SEQUENCE_LENGTH, LRU_WIDTH), jnp.float32, 0.5, 1.5)
    return -0.5 / SEQUENCE_LENGTH * multiplier[:, :, None] * random_jitter + spike_log_values(key_rows[2], 2)[:, :, None]


def block_scale(stream_key, dims, pieces, low, largest):
    loudness, own = 1.0, jax.random.fold_in(stream_key, 6)
    for dim, shards_of in pieces:
        draws = jnp.exp(jax.random.uniform(jax.random.fold_in(own, dim), (shards_of,), jnp.float32, low / len(pieces), largest / len(pieces)))
        loudness = loudness * jnp.repeat(draws, dims[dim] // shards_of).reshape([-1 if axis == dim else 1 for axis in range(len(dims))])
    return loudness


def normal_values(stream_key, extent, width, limit, shards=(), kind=jnp.bfloat16):
    result = width * jax.random.normal(stream_key, extent, jnp.float32)
    if shards:
        result = result * block_scale(stream_key, extent, shards, -0.22, 0.18)
    return jnp.clip(result, -limit, limit).astype(kind)


def setup_inputs(seed: int = 0) -> dict:
    key_of = jax.random.split(jax.random.key(seed), 20)
    inputs = normal_values(key_of[0], (SEQS, SEQUENCE_LENGTH, D), 1.0, 6.0, ((1, 8),))
    norm_gain = jnp.clip(1.0 + 0.18 * jax.random.normal(key_of[1], (D,), jnp.float32), 0.1, 1.9)
    query_weight = normal_values(key_of[2], (D, ATT_WIDTH), D ** -0.5, 0.125, ((0, 8), (1, 4)))
    key_weight = normal_values(key_of[3], (D, KV_WIDTH), D ** -0.5, 0.125, ((0, 8), (1, 4)))
    value_weight = normal_values(key_of[4], (D, KV_WIDTH), D ** -0.5, 0.125, ((0, 8), (1, 4)))
    query_gain = draw_query_gain(jax.random.fold_in(key_of[19], 71), 0)
    key_gain = jnp.clip(1.0 + 0.18 * jax.random.normal(key_of[6], (HEAD_DIM,), jnp.float32), 0.1, 1.9)
    forget_cache = draw_forget_cache(jax.random.fold_in(key_of[19], 71), 0)
    rec_in_weight = normal_values(key_of[8], (D, LRU_WIDTH), D ** -0.5, 0.125, ((0, 8), (1, 4)))
    rec_gate_weight = normal_values(key_of[9], (D, LRU_WIDTH), D ** -0.5, 0.125, ((0, 8), (1, 4)))
    conv_weight = normal_values(key_of[10], (CONV_TAPS, LRU_WIDTH), CONV_TAPS ** -0.5, 3.0, ((1, 4),))
    decay_gate_weight = normal_values(key_of[11], (LRU_BLOCKS, LRU_BLOCK, LRU_BLOCK), LRU_BLOCK ** -0.5, 0.75, ((0, 4),))
    input_gate_weight = normal_values(key_of[12], (LRU_BLOCKS, LRU_BLOCK, LRU_BLOCK), LRU_BLOCK ** -0.5, 0.75, ((0, 4),))
    decay_param = draw_decay_param(jax.random.fold_in(key_of[19], 71), 0)
    decay_extra = draw_decay_extra(jax.random.fold_in(key_of[19], 71), 0)
    attn_out_gain = jnp.clip(1.0 + 0.18 * jax.random.normal(key_of[15], (ATT_WIDTH,), jnp.float32), 0.1, 1.9)
    rec_out_gain = jnp.clip(1.0 + 0.18 * jax.random.normal(key_of[16], (LRU_WIDTH,), jnp.float32), 0.1, 1.9)
    out_att_weight = normal_values(key_of[17], (ATT_WIDTH, D), D ** -0.5, 0.125, ((0, 4),))
    out_rec_weight = normal_values(key_of[18], (LRU_WIDTH, D), D ** -0.5, 0.125, ((0, 4),))
    return {"inputs": inputs, "norm_gain": norm_gain, "query_weight": query_weight, "key_weight": key_weight, "value_weight": value_weight, "query_gain": query_gain, "key_gain": key_gain, "forget_cache": forget_cache, "rec_in_weight": rec_in_weight, "rec_gate_weight": rec_gate_weight, "conv_weight": conv_weight, "decay_gate_weight": decay_gate_weight, "input_gate_weight": input_gate_weight, "decay_param": decay_param, "decay_extra": decay_extra, "attn_out_gain": attn_out_gain, "rec_out_gain": rec_out_gain, "out_att_weight": out_att_weight, "out_rec_weight": out_rec_weight}


lru_const = 8.0
norm_eps = 1e-06

def rms_scale(values, gain):
    multiplier = lax.rsqrt(lax.optimization_barrier(jnp.mean(values * values, axis=-1, keepdims=True)) + norm_eps)
    return values * multiplier * gain

def merge_state(earlier, later):
    return (earlier[0] * later[0], later[0] * earlier[1] + later[1])

def attention(queries, key_heads, value_heads, forget_cache):
    seq_count, kv_count, head_group, length, head_dim = queries.shape
    block_size = 512
    while length % block_size:
        block_size //= 2
    scaling = head_dim ** (-0.5)
    gates = forget_cache.reshape(seq_count, kv_count, head_group, length)
    offsets = jnp.arange(block_size, dtype=jnp.int32)

    def one_block(index):
        first = index * block_size
        query_block = lax.dynamic_slice_in_dim(queries, first, block_size, 3).astype(jnp.float32)
        query_gates = lax.dynamic_slice_in_dim(gates, first, block_size, 3)
        query_pos = first + offsets

        def one_step(block_index, carried):
            top_score, totals, accum = carried
            key_first = block_index * block_size
            key_block = lax.dynamic_slice_in_dim(key_heads, key_first, block_size, 2).astype(jnp.float32)
            value_block = lax.dynamic_slice_in_dim(value_heads, key_first, block_size, 2).astype(jnp.float32)
            key_gates = lax.dynamic_slice_in_dim(gates, key_first, block_size, 3)
            scores = jnp.einsum('bhgqd,bhkd->bhgqk', query_block, key_block) * scaling
            scores = scores + query_gates[..., :, None] - key_gates[..., None, :]
            visible = query_pos[:, None] >= (key_first + offsets)[None, :]
            scores = jnp.where(visible, scores, -jnp.inf)
            new_top = jnp.maximum(top_score, lax.optimization_barrier(jnp.max(scores, axis=-1)))
            weights = jnp.exp(scores - new_top[..., None])
            fading = jnp.exp(top_score - new_top)
            rounded = lax.optimization_barrier(weights.astype(jnp.bfloat16)).astype(jnp.float32)
            totals = totals * fading + lax.optimization_barrier(jnp.sum(weights, axis=-1))
            accum = accum * fading[..., None] + jnp.einsum('bhgqk,bhkd->bhgqd', rounded, value_block)
            return (new_top, totals, accum)
        start_state = (jnp.full((seq_count, kv_count, head_group, block_size), -jnp.inf, jnp.float32), jnp.zeros((seq_count, kv_count, head_group, block_size), jnp.float32), jnp.zeros((seq_count, kv_count, head_group, block_size, head_dim), jnp.float32))
        top_score, totals, accum = lax.fori_loop(0, index + 1, one_step, start_state)
        return accum / totals[..., None]
    return lax.map(one_block, jnp.arange(length // block_size, dtype=jnp.int32))

def reference(inputs, norm_gain, query_weight, key_weight, value_weight, query_gain, key_gain, forget_cache, rec_in_weight, rec_gate_weight, conv_weight, decay_gate_weight, input_gate_weight, decay_param, decay_extra, attn_out_gain, rec_out_gain, out_att_weight, out_rec_weight):
    seq_count, length, model_width = inputs.shape
    row_count = seq_count * length
    head_group = ATT_HEADS // KV_HEADS
    flat_rows = inputs.reshape(row_count, model_width).astype(jnp.float32)
    normed = rms_scale(flat_rows, norm_gain).astype(jnp.bfloat16)

    def project(weight):
        return jnp.dot(normed, weight, preferred_element_type=jnp.float32)
    query_proj = project(query_weight)
    key_proj = project(key_weight)
    gate_proj = project(rec_gate_weight)
    value_proj = project(value_weight).astype(jnp.bfloat16)
    rec_in = project(rec_in_weight).astype(jnp.bfloat16)
    queries = rms_scale(query_proj.reshape(seq_count, length, ATT_HEADS, HEAD_DIM), query_gain).astype(jnp.bfloat16)
    queries = queries.transpose(0, 2, 1, 3).reshape(seq_count, KV_HEADS, head_group, length, HEAD_DIM)
    key_heads = rms_scale(key_proj.reshape(seq_count, length, KV_HEADS, HEAD_DIM), key_gain).astype(jnp.bfloat16)
    key_heads = key_heads.transpose(0, 2, 1, 3)
    value_heads = value_proj.reshape(seq_count, length, KV_HEADS, HEAD_DIM).transpose(0, 2, 1, 3)
    blocks = attention(queries, key_heads, value_heads, forget_cache)
    attended = blocks.transpose(1, 0, 4, 2, 3, 5).reshape(row_count, ATT_HEADS, HEAD_DIM)
    att_normed = rms_scale(attended, attn_out_gain.reshape(ATT_HEADS, HEAD_DIM)).astype(jnp.bfloat16)
    att_normed = att_normed.reshape(row_count, ATT_WIDTH)
    rec_seq = rec_in.reshape(seq_count, length, LRU_WIDTH)
    padded = jnp.pad(rec_seq, ((0, 0), (CONV_TAPS - 1, 0), (0, 0)))
    conv = jnp.zeros((seq_count, length, LRU_WIDTH), jnp.float32)
    for tap in range(CONV_TAPS):
        conv = conv + padded[:, tap:tap + length].astype(jnp.float32) * conv_weight[tap].astype(jnp.float32)
    conv = conv.astype(jnp.bfloat16)
    conv_wide = conv.astype(jnp.float32)
    grouped = conv_wide.reshape(seq_count, length, LRU_BLOCKS, LRU_BLOCK)
    gate_decay = jnp.einsum('bsnd,nde->bsne', grouped, decay_gate_weight.astype(jnp.float32))
    gate_decay = gate_decay.reshape(seq_count, length, LRU_WIDTH)
    gate_input = jnp.einsum('bsnd,nde->bsne', grouped, input_gate_weight.astype(jnp.float32))
    gate_input = gate_input.reshape(seq_count, length, LRU_WIDTH)
    log_decay = -lru_const * jax.nn.sigmoid(gate_decay) * jax.nn.softplus(-decay_param) + decay_extra
    drive = jnp.sqrt(-jnp.expm1(2.0 * log_decay)) * jax.nn.sigmoid(gate_input) * conv_wide
    unused_decay, state = lax.associative_scan(merge_state, (jnp.exp(log_decay), drive), axis=1)
    gated = state * jax.nn.gelu(gate_proj.reshape(seq_count, length, LRU_WIDTH))
    rec_normed = rms_scale(gated.reshape(row_count, LRU_BLOCKS, LRU_BLOCK), rec_out_gain.reshape(LRU_BLOCKS, LRU_BLOCK)).astype(jnp.bfloat16)
    rec_normed = rec_normed.reshape(row_count, LRU_WIDTH)
    mixed = jnp.dot(att_normed, out_att_weight, preferred_element_type=jnp.float32)
    mixed = mixed + jnp.dot(rec_normed, out_rec_weight, preferred_element_type=jnp.float32)
    return mixed.astype(jnp.bfloat16).reshape(seq_count, length, model_width)
```

```python
import functools

import jax
import jax.numpy as jnp
from jax import lax
from jax.experimental import pallas as pl
from jax.experimental.pallas import tpu as pltpu
from jax.sharding import PartitionSpec as P

LRU_CONST = 8.0
EPS = 1e-06
F32 = jnp.float32
BF16 = jnp.bfloat16
MESH = pl.DeviceIdType.MESH


def group_rms(values, gain, width):
    parts = []
    for start in range(0, values.shape[1], width):
        part = values[:, start : start + width]
        scale = lax.rsqrt(jnp.mean(part * part, axis=-1, keepdims=True) + EPS)
        parts.append(part * scale)
    return jnp.concatenate(parts, axis=1) * gain


def one_minus_exp(y):
    series = y * (1 + y / 2 * (1 + y / 3 * (1 + y / 4 * (1 + y / 5 * (1 + y / 6 * (1 + y / 7))))))
    return -jnp.where(y > -0.4, series, jnp.exp(y) - 1.0)


def softplus(x):
    u = jnp.exp(-jnp.abs(x))
    s = u / (2.0 + u)
    q = s * s
    series = 1.0 / 17
    for odd in (15, 13, 11, 9, 7, 5, 3, 1):
        series = series * q + 1.0 / odd
    return jnp.maximum(x, 0.0) + 2.0 * s * series


def sigmoid(x):
    return 1.0 / (1.0 + jnp.exp(-x))


def gelu(x):
    return 0.5 * x * (1.0 + jnp.tanh(0.7978845608028654 * (x + 0.044715 * x * x * x)))


def dot(a, b):
    return jnp.dot(a, b, preferred_element_type=F32)


def kernel(
    dims,
    x_ref, norm_ref, wq_ref, wk_ref, wv_ref, qg_ref, kg_ref, fc_ref, wr_ref, wg_ref, cw_ref,
    dgw_ref, igw_ref, dp_ref, de_ref, ag_ref, rg_ref, oa_ref, or_ref,
    out_ref,
    normed, kvw, rw, qw, gw, kv_all, rin, halo, st_all, halves, sums, parts, got,
    zs, zr, fs, fr, hs, hr, ss, sr, ps, pr, qs, qr,
):
    n, nt, seqs, span, head_dim, block, length = dims
    rows = seqs * span
    no, nto = n // 2, nt // 2
    me = lax.axis_index("sp")
    outer, inner = lax.div(me, 2), lax.rem(me, 2)
    mate = outer * 2 + (1 - inner)
    tme = lax.axis_index("tp")
    touter, tinner = lax.div(tme, 2), lax.rem(tme, 2)
    tmate = touter * 2 + (1 - tinner)
    kr = wq_ref.shape[0]
    kvc = wk_ref.shape[1]
    att_local = wq_ref.shape[1] // head_dim
    kv_local = kvc // head_dim
    hg = att_local // kv_local
    taps = cw_ref.shape[0]

    def to_outer(d):
        return lax.rem(outer + d, no) * 2 + inner

    def from_outer(d):
        return lax.rem(outer + no - d, no) * 2 + inner

    barrier = pltpu.get_barrier_semaphore()
    for d in range(1, n):
        pl.semaphore_signal(barrier, inc=1, device_id={"sp": lax.rem(me + d, n)}, device_id_type=MESH)
    for d in range(1, nt):
        pl.semaphore_signal(barrier, inc=1, device_id={"tp": lax.rem(tme + d, nt)}, device_id_type=MESH)

    def slot(ref, who):
        return ref.at[pl.ds(pl.multiple_of(who * kr, kr), kr), :]

    own_rows = pl.ds(pl.multiple_of(me * kr, kr), kr)
    kvw[own_rows, :] = jnp.concatenate([wk_ref[...], wv_ref[...]], axis=1)
    rw[own_rows, :] = wr_ref[...]
    qw[own_rows, :] = wq_ref[...]
    gw[own_rows, :] = wg_ref[...]
    pl.semaphore_wait(barrier, n - 1 + nt - 1)

    buffers = (kvw, rw, qw, gw, kv_all)
    sources = (None, wr_ref, wq_ref, wg_ref, None)

    def place(c, who):
        return kv_all.at[who] if c == 4 else slot(buffers[c], who)

    def origin(c):
        return place(c, me) if sources[c] is None else sources[c]

    def outward(c, d, who, src):
        return pltpu.make_async_remote_copy(
            src_ref=src, dst_ref=place(c, who), send_sem=zs.at[c, d - 1], recv_sem=zr.at[c, d - 1],
            device_id={"sp": to_outer(d)}, device_id_type=MESH,
        )

    def across(c, d, who, src):
        return pltpu.make_async_remote_copy(
            src_ref=src, dst_ref=place(c, who), send_sem=fs.at[c, d], recv_sem=fr.at[c, d],
            device_id={"sp": mate}, device_id_type=MESH,
        )

    def send_own(c):
        for d in range(1, no):
            outward(c, d, me, origin(c)).start()
        across(c, 0, me, origin(c)).start()

    def forward(c):
        for d in range(1, no):
            who = from_outer(d)
            outward(c, d, who, place(c, who)).wait_recv()
            across(c, d, who, place(c, who)).start()

    def finish(c):
        for d in range(no):
            who = lax.rem(outer + no - d, no) * 2 + (1 - inner)
            across(c, d, who, place(c, who)).wait_recv()

    def drain(c):
        for d in range(1, no):
            outward(c, d, me, origin(c)).wait_send()
        across(c, 0, me, origin(c)).wait_send()
        for d in range(1, no):
            who = from_outer(d)
            across(c, d, who, place(c, who)).wait_send()

    send_own(0)
    send_own(1)
    send_own(2)

    x = x_ref[...].astype(F32)
    scale = lax.rsqrt(jnp.mean(x * x, axis=-1, keepdims=True) + EPS)
    normed[...] = (x * scale * norm_ref[...]).astype(BF16)

    forward(0)
    forward(1)
    finish(0)
    kv = dot(normed[...], kvw[...])
    keys = jnp.concatenate(
        [group_rms(kv[:, g * head_dim : (g + 1) * head_dim], kg_ref[...], head_dim) for g in range(kv_local)], axis=1
    )
    kv_all[me] = jnp.concatenate([keys, kv[:, kvc:]], axis=1).astype(BF16)
    send_own(4)

    finish(1)
    rec = dot(normed[...], rw[...]).astype(BF16).astype(F32)
    nxt, prv = lax.rem(me + 1, n), lax.rem(me + n - 1, n)
    for b in range(seqs):
        rin[b, pl.ds(8, span), :] = rec[b * span : (b + 1) * span]
    for b in range(seqs):
        halo[0, pl.ds(b * 8, 8), :] = rin[b, pl.ds(span, 8), :]
    halo_copy = pltpu.make_async_remote_copy(
        src_ref=halo.at[0], dst_ref=halo.at[1], send_sem=hs, recv_sem=hr,
        device_id={"sp": nxt}, device_id_type=MESH,
    )
    halo_copy.start()
    send_own(3)

    forward(2)
    forward(4)

    halo_copy.wait()
    first = me == 0
    for b in range(seqs):
        edge = halo[1, pl.ds(b * 8, 8), :]
        rin[b, pl.ds(0, 8), :] = jnp.where(first, jnp.zeros_like(edge), edge)
    convs = []
    for b in range(seqs):
        conv = jnp.zeros((span, rw.shape[1]), F32)
        for tap in range(taps):
            conv = conv + rin[b, pl.ds(8 - (taps - 1) + tap, span), :] * cw_ref[pl.ds(tap, 1), :]
        convs.append(conv)
    conv = jnp.concatenate(convs, axis=0).astype(BF16)
    nb, lb = dgw_ref.shape[0], dgw_ref.shape[1]
    gate_decay = jnp.concatenate([dot(conv[:, i * lb : (i + 1) * lb], dgw_ref[i]) for i in range(nb)], axis=1)
    gate_input = jnp.concatenate([dot(conv[:, i * lb : (i + 1) * lb], igw_ref[i]) for i in range(nb)], axis=1)
    log_decay = -LRU_CONST * sigmoid(gate_decay) * softplus(-dp_ref[...]) + de_ref[...]
    state = jnp.sqrt(one_minus_exp(2.0 * log_decay)) * sigmoid(gate_input) * conv.astype(F32)
    decay = jnp.exp(log_decay)
    time = lax.rem(lax.broadcasted_iota(jnp.int32, state.shape, 0), span)
    shift = 1
    while shift < span:
        seen = time >= shift
        state = state + decay * jnp.where(seen, pltpu.roll(state, shift, 0), 0.0)
        decay = decay * jnp.where(seen, pltpu.roll(decay, shift, 0), 1.0)
        shift *= 2
    ends = [decay[(b + 1) * span - 1 : (b + 1) * span] for b in range(seqs)]
    ends += [state[(b + 1) * span - 1 : (b + 1) * span] for b in range(seqs)]
    for i, row in enumerate(ends):
        st_all[me, pl.ds(i, 1), :] = row
    def state_copy(d, who):
        return pltpu.make_async_remote_copy(
            src_ref=st_all.at[who], dst_ref=st_all.at[who], send_sem=ss.at[d - 1], recv_sem=sr.at[d - 1],
            device_id={"sp": lax.rem(me + d, n)}, device_id_type=MESH,
        )

    for d in range(1, n):
        state_copy(d, me).start()

    finish(2)
    scaling = head_dim ** (-0.5)
    query = dot(normed[...], qw[...])
    queries = [
        (group_rms(query[:, h * head_dim : (h + 1) * head_dim], qg_ref[...], head_dim).astype(BF16) * scaling).astype(BF16)
        for h in range(att_local)
    ]
    finish(4)
    shards = block // span
    first_pos = me * span
    query_pos = first_pos + lax.broadcasted_iota(jnp.int32, (span, block), 0)
    key_off = lax.broadcasted_iota(jnp.int32, (span, block), 1)
    needed = lax.div(first_pos + span + block - 1, block)
    attended = []
    for b in range(seqs):
        heads = []
        for h in range(att_local):
            g = h // hg
            q = queries[h][b * span : (b + 1) * span]

            def step(j, carried, q=q, b=b, h=h, g=g):
                top, total, accum = carried
                kvb = kv_all[pl.ds(j * shards, shards), pl.ds(b * span, span), :].reshape(block, 2 * kvc)
                kb = kvb[:, g * head_dim : (g + 1) * head_dim]
                vb = kvb[:, kvc + g * head_dim : kvc + (g + 1) * head_dim]
                s = lax.dot_general(q, kb, (((1,), (1,)), ((), ())), preferred_element_type=F32)
                s = s - fc_ref[b, pl.ds(h, 1), pl.ds(pl.multiple_of(j * block, block), block)]
                s = jnp.where(query_pos >= key_off + j * block, s, -jnp.inf)
                new_top = jnp.maximum(top, jnp.max(s, axis=-1, keepdims=True))
                w = jnp.exp(s - new_top)
                fade = jnp.exp(top - new_top)
                total = total * fade + jnp.sum(w, axis=-1, keepdims=True)
                return new_top, total, accum * fade + dot(w.astype(BF16), vb)

            start = (jnp.full((span, 1), -1e30, F32), jnp.zeros((span, 1), F32), jnp.zeros((span, head_dim), F32))
            if length == block:
                top, total, accum = step(0, start)
            else:
                top, total, accum = lax.fori_loop(0, needed, step, start)
            value = accum / total
            value = value * lax.rsqrt(jnp.mean(value * value, axis=-1, keepdims=True) + EPS)
            heads.append(value)
        attended.append(jnp.concatenate(heads, axis=1))
    halves[0] = (jnp.concatenate(attended, axis=0) * ag_ref[...]).astype(BF16)

    forward(3)
    for d in range(1, n):
        state_copy(d, lax.rem(me + n - d, n)).wait_recv()

    def enter(j, e):
        block_state = st_all[j]
        return block_state[0:seqs] * e + block_state[seqs : 2 * seqs]

    entering = lax.fori_loop(0, me, enter, jnp.zeros((seqs, rw.shape[1]), F32))
    whole_state = jnp.concatenate(
        [
            state[b * span : (b + 1) * span] + decay[b * span : (b + 1) * span] * entering[b : b + 1]
            for b in range(seqs)
        ],
        axis=0,
    )
    finish(3)
    gated = whole_state * gelu(dot(normed[...], gw[...]))
    halves[1] = group_rms(gated, rg_ref[...], lb).astype(BF16)

    cols = out_ref.shape[1]

    def piece(who):
        span_cols = pl.ds(pl.multiple_of(who * cols, cols), cols)
        return dot(halves[0], oa_ref[:, span_cols]) + dot(halves[1], or_ref[:, span_cols])

    def to_mate(s):
        return pltpu.make_async_remote_copy(
            src_ref=sums.at[s], dst_ref=parts.at[s], send_sem=ps.at[s], recv_sem=pr.at[s],
            device_id={"tp": tmate}, device_id_type=MESH,
        )

    def to_far(d):
        return pltpu.make_async_remote_copy(
            src_ref=sums.at[nto + d - 1], dst_ref=got.at[d - 1], send_sem=qs.at[d - 1], recv_sem=qr.at[d - 1],
            device_id={"tp": lax.rem(touter + d, nto) * 2 + tinner}, device_id_type=MESH,
        )

    for s in list(range(1, nto)) + [0]:
        sums[s] = piece(lax.rem(touter + s, nto) * 2 + (1 - tinner)).astype(BF16)
        to_mate(s).start()
    for d in range(1, nto):
        mine = piece(lax.rem(touter + d, nto) * 2 + tinner)
        to_mate(d).wait_recv()
        sums[nto + d - 1] = (mine + parts[d].astype(F32)).astype(BF16)
        to_far(d).start()
    mine = piece(tme)
    to_mate(0).wait_recv()
    mine = mine + parts[0].astype(F32)
    for d in range(1, nto):
        to_far(d).wait_recv()
        mine = mine + got[d - 1].astype(F32)
    out_ref[...] = mine.astype(BF16)

    for c in range(5):
        drain(c)
    for d in range(1, n):
        state_copy(d, me).wait_send()
    for s in range(nto):
        to_mate(s).wait_send()
    for d in range(1, nto):
        to_far(d).wait_send()


def body(
    n, nt,
    inputs, norm_gain, query_weight, key_weight, value_weight, query_gain, key_gain, forget_cache,
    rec_in_weight, rec_gate_weight, conv_weight, decay_gate_weight, input_gate_weight, decay_param,
    decay_extra, attn_out_gain, rec_out_gain, out_att_weight, out_rec_weight,
):
    seqs, span, width = inputs.shape
    rows = seqs * span
    head_dim = query_gain.shape[0]
    length = forget_cache.shape[2]
    channels = rec_in_weight.shape[1]
    qc, kvc = query_weight.shape[1], key_weight.shape[1]
    cols = out_att_weight.shape[1] // nt
    block = span
    while block * 2 <= 1024 and length % (block * 2) == 0:
        block *= 2
    no, nto = n // 2, nt // 2
    dma = pltpu.SemaphoreType.DMA
    vmem = pl.BlockSpec(memory_space=pltpu.VMEM)
    out = pl.pallas_call(
        functools.partial(kernel, (n, nt, seqs, span, head_dim, block, length)),
        out_shape=jax.ShapeDtypeStruct((rows, cols), BF16),
        in_specs=[vmem] * 19,
        out_specs=vmem,
        scratch_shapes=[
            pltpu.VMEM((rows, width), BF16),
            pltpu.VMEM((width, 2 * kvc), BF16),
            pltpu.VMEM((width, channels), BF16),
            pltpu.VMEM((width, qc), BF16),
            pltpu.VMEM((width, channels), BF16),
            pltpu.VMEM((n, rows, 2 * kvc), BF16),
            pltpu.VMEM((seqs, span + 8, channels), F32),
            pltpu.VMEM((2, seqs * 8, channels), F32),
            pltpu.VMEM((n, -(-2 * seqs // 8) * 8, channels), F32),
            pltpu.VMEM((2, rows, channels), BF16),
            pltpu.VMEM((2 * nto, rows, cols), BF16),
            pltpu.VMEM((nto, rows, cols), BF16),
            pltpu.VMEM((nto, rows, cols), BF16),
            dma((5, no)), dma((5, no)), dma((5, no)), dma((5, no)),
            dma, dma, dma((n,)), dma((n,)),
            dma((nto,)), dma((nto,)), dma((nto,)), dma((nto,)),
        ],
        compiler_params=pltpu.CompilerParams(
            collective_id=0, has_side_effects=True, vmem_limit_bytes=60 * 1024 * 1024
        ),
    )(
        inputs.reshape(rows, width), norm_gain.reshape(1, width), query_weight, key_weight, value_weight,
        query_gain.reshape(1, head_dim), key_gain.reshape(1, head_dim), forget_cache,
        rec_in_weight, rec_gate_weight, conv_weight.astype(F32), decay_gate_weight, input_gate_weight,
        decay_param.reshape(1, channels), decay_extra.reshape(rows, channels),
        attn_out_gain.reshape(1, qc), rec_out_gain.reshape(1, channels), out_att_weight, out_rec_weight,
    )
    return out.reshape(seqs, span, cols)


def solution(mesh):
    return jax.shard_map(
        functools.partial(body, mesh.shape["sp"], mesh.shape["tp"]),
        mesh=mesh,
        in_specs=(
            P(None, "sp", None), P(), P("sp", "tp"), P("sp", "tp"), P("sp", "tp"), P(), P(),
            P(None, "tp", None), P("sp", "tp"), P("sp", "tp"), P(None, "tp"), P("tp", None, None),
            P("tp", None, None), P("tp"), P(None, "sp", "tp"), P("tp"), P("tp"), P("tp", None), P("tp", None),
        ),
        out_specs=P(None, "sp", "tp"),
        check_vma=False,
    )
```
